32 devices in a mesh: ep: 4 (over y, x), tp: 8 (over z, core).
Axes of the slice: x: 2, y: 2, z: 4, core: 2. Of those that a mesh axis runs over, the one named last changes fastest.
Arguments:
- query_heads: bfloat16 [16384, 4096], P('ep', 'tp'), may hold values from -6 to 6
- key_heads: bfloat16 [16384, 4096], P('ep', 'tp'), may hold values from -6 to 6
- value_heads: bfloat16 [16384, 4096], P('ep', 'tp'), may hold values from -6 to 6
- log_decay: float32 [16384, 16], P('ep', 'tp'), may hold values from -1 to 0
- head_gain: float32 [4096], P('tp'), may hold values from 0.1 to 1.9
- expert_input: bfloat16 [3072, 2048], P(('ep', 'tp')), may hold values from -400 to 400
- input_gain: float32 [2048], replicated, may hold values from 0.1 to 1.9
- specialist_choices: int32 [3072, 2], P(('ep', 'tp')), may hold values from 0 to 7, all different within a row; in each aligned block of 96 rows (0 to 95, 96 to 191, ...) at most 25 rows name the same one
- route_weight: float32 [3072, 2], P(('ep', 'tp')), may hold values from 0.1 to 1
- gate_weight: bfloat16 [2048, 16384], P(None, ('ep', 'tp')), may hold values from -0.5 to 0.5
- up_weight: bfloat16 [2048, 16384], P(None, ('ep', 'tp')), may hold values from -0.5 to 0.5
- down_weight: bfloat16 [16384, 2048], P(('ep', 'tp')), may hold values from -0.015625 to 0.015625
Outputs:
- mixer_out: bfloat16 [16384, 4096], P('ep', 'tp')
- expert_out: bfloat16 [3072, 2048], P(('ep', 'tp'))
The draws below stay inside these ranges and needn't reach their ends.
Inputs may be any that keep to these rules, and one draw needn't show every extreme that they name: `specialist_choices`: in the rows of one device no expert is named more than 25 times, a bound that some block reaches.
All inputs are finite; a program needn't handle non-finite values.
Results may differ from the reference program's by a relative error of at most 0.0076.
Values may be sent and summed in bfloat16 or wider, within the bound.
A program may use at most 128 MiB of HBM per device.

```python
import math
import jax
import jax.numpy as jnp
import numpy as np
from jax import lax

D = 2048
HEADS = 16
DH = 256
FF = 2048
EXP_DEV = 2
TOP_K = 2
BLK = 512
SEG_DEV = 4096
TOK_B = 96
SEQUENCE_LENGTH = 16384
EXPERTS = 8
TOKENS_B = 3072
CAP = 25
N_EP = 4
N_TP = 8


def draw_log_decay(key, part):
    streams = jax.random.split(jax.random.fold_in(key, 11), 6)
    length = SEG_DEV * N_EP
    share = 0.5
    fast = jax.random.uniform(streams[0], (HEADS,), jnp.float32) < share
    fast_rate = jnp.exp(jax.random.uniform(streams[1], (HEADS,), jnp.float32, math.log(1.0 / 100.0), math.log(1.0 / 30.0)))
    slow_rate = jax.random.uniform(streams[2], (HEADS,), jnp.float32, 0.05, 0.3) / length
    forgetting_speeds = jnp.where(fast, fast_rate, slow_rate)
    block_count = length // BLK
    multiplier_coefficient = jnp.exp(jax.random.uniform(streams[3], (block_count, HEADS), jnp.float32, -math.log(2.0), math.log(2.0)))
    multiplier_coefficient = jnp.repeat(multiplier_coefficient, BLK, axis=0)
    spots = jax.random.randint(streams[4], (2,), 0, length)
    overflow_discards = jnp.log(jax.random.uniform(streams[5], (2, HEADS), jnp.float32, 0.5, 0.8))
    positions = jnp.arange(length)
    specialist_tallies = (positions[:, None] == spots[None, :]).astype(jnp.float32)
    token_batches = jnp.sum(specialist_tallies[:, :, None] * overflow_discards[None, :, :], axis=1)
    return (-forgetting_speeds[None, :] * multiplier_coefficient + token_batches).astype(jnp.float32)


def draw_expert_input(key, part):
    streams = jax.random.split(jax.random.fold_in(key, 23), 3)
    row_scale = jnp.exp(jax.random.uniform(streams[0], (TOKENS_B, 1), jnp.float32, 0.0, math.log(10.0)))
    column_scale = jnp.exp(jax.random.uniform(streams[1], (1, D), jnp.float32, 0.0, math.log(10.0)))
    base = jnp.clip(jax.random.normal(streams[2], (TOKENS_B, D), jnp.float32), -4.0, 4.0)
    return (base * row_scale * column_scale).astype(jnp.bfloat16)


def block_levels(key, shape, shards, smallest, high):
    def one(position, parts):
        draws = jax.random.uniform(jax.random.fold_in(jax.random.fold_in(key, 6), position), (parts,), jnp.float32, smallest / len(shards), high / len(shards))
        return jnp.repeat(jnp.exp(draws), shape[position] // parts).reshape((-1,) + (1,) * (len(shape) - position - 1))

    loudness = one(*shards[0])
    for cut in shards[1:]:
        loudness = loudness * one(*cut)
    return loudness


def deal_out(own_key, own, number, rows, count, top, limit, lean):
    order = jax.random.permutation(own_key, count)
    crowded, usual = shares(count, rows * top, limit, lean, True), shares(count, rows * top, limit, lean, False)
    places = jnp.arange(count)

    def named(sizes, offset_by):
        used = int((sizes > 0).sum())
        fixed = max(1, used // 4)
        moved = fixed + (places - fixed + offset_by * (used - fixed)) % max(1, count - fixed)
        return jnp.zeros((count,), jnp.int32).at[order[jnp.where(places < fixed, places, moved)]].set(jnp.asarray(sizes, jnp.int32))

    sizes = jnp.where(number % 4 == 0, named(crowded, number // 4), named(usual, number - number // 4 - 1))
    mixed = jax.random.permutation(jax.random.fold_in(own, 3), count)
    giver, taker = mixed[0:count // 2 * 2:2], mixed[1:count // 2 * 2:2]
    room = jnp.minimum(sizes[giver] - 1, limit - sizes[taker]) // 2
    room = jnp.where((giver == order[0]) | (taker == order[0]) | (sizes[taker] == 0), 0, jnp.maximum(room, 0))
    moved = jax.random.randint(jax.random.fold_in(own, 4), (count // 2,), 0, 1 << 20) % (room + 1)
    sizes = sizes.at[giver].add(-moved).at[taker].add(moved)
    labels = jnp.searchsorted(jnp.cumsum(sizes), jnp.arange(rows * top), side="right").astype(jnp.int32)
    listing = labels.reshape(top, rows).T
    listing = listing[jax.random.permutation(jax.random.fold_in(own, 1), rows)]
    offset_by = jax.random.randint(jax.random.fold_in(own, 2), (rows, 1), 0, top)
    return jnp.take_along_axis(listing, (jnp.arange(top)[None, :] + offset_by) % top, axis=1)


def shares(amount, total, limit, lean, full):
    weights = [(1 << 20) // math.isqrt(rank ** lean) + 1 for rank in range(1, amount + 1)]
    largest = limit if full else min(limit, max(-(-total // amount), total * weights[0] // sum(weights)))
    least = 1 if total - largest >= amount - 1 else 0
    counts, spare = [largest] + [least] * (amount - 1), total - largest - least * (amount - 1)
    while spare > 0:
        movable = [i for i in range(1, amount) if counts[i] < largest] or [i for i in range(1, amount) if counts[i] < limit]
        whole, budget = sum([weights[i] for i in movable]), spare
        for i in movable:
            addition = min(limit - counts[i], max(1, budget * weights[i] // whole), spare)
            counts[i] = counts[i] + addition
            spare = spare - addition
    return np.array(counts)


def normal_values(rng, dims, spread, most, shards=(), held_as=jnp.bfloat16):
    array = spread * jax.random.normal(rng, dims, jnp.float32)
    if shards:
        array = array * block_levels(rng, dims, shards, -0.22, 0.18)
    return jnp.clip(array, -most, most).astype(held_as)


def setup_inputs(seed: int = 0) -> dict:
    keys = jax.random.split(jax.random.key(seed), 13)
    query_heads = normal_values(keys[0], (SEQUENCE_LENGTH, HEADS * DH), 1.0, 6.0, ((0, 4), (1, 8)))
    key_heads = normal_values(keys[1], (SEQUENCE_LENGTH, HEADS * DH), 1.0, 6.0, ((0, 4), (1, 8)))
    value_heads = normal_values(keys[2], (SEQUENCE_LENGTH, HEADS * DH), 1.0, 6.0, ((0, 4), (1, 8)))
    log_decay = draw_log_decay(jax.random.fold_in(keys[12], 71), 0)
    head_gain = jnp.clip(1.0 + 0.18 * jax.random.normal(keys[4], (HEADS * DH,), jnp.float32), 0.1, 1.9)
    expert_input = draw_expert_input(jax.random.fold_in(keys[12], 71), 0)
    input_gain = jnp.clip(1.0 + 0.18 * jax.random.normal(keys[6], (D,), jnp.float32), 0.1, 1.9)
    specialist_choices_keys = jax.random.split(jax.random.fold_in(keys[7], 1), TOKENS_B // TOK_B)
    specialist_choices_turns = jax.random.permutation(jax.random.fold_in(keys[7], 3), TOKENS_B // TOK_B)
    specialist_choices = jax.vmap(lambda own, number: deal_out(jax.random.fold_in(keys[7], 2), own, number, TOK_B, EXPERTS, TOP_K, CAP, 1))(specialist_choices_keys, specialist_choices_turns).reshape((TOKENS_B, TOP_K))
    route_weight = jnp.clip(jnp.exp(math.log(1.0) - 2.3025851 * jax.random.uniform(keys[8], (TOKENS_B, TOP_K), jnp.float32) ** block_levels(keys[8], (TOKENS_B, TOP_K), ((0, 32),), -0.2, 0.2)), 0.1, 1.0)
    gate_weight = normal_values(keys[9], (D, EXPERTS * FF), (D // 16) ** -0.5, 0.5, ((1, 32),))
    up_weight = normal_values(keys[10], (D, EXPERTS * FF), (D // 16) ** -0.5, 0.5, ((1, 32),))
    down_weight = normal_values(keys[11], (EXPERTS * FF, D), (FF * 64) ** -0.5, 0.015625, ((0, 32),))
    return {"query_heads": query_heads, "key_heads": key_heads, "value_heads": value_heads, "log_decay": log_decay, "head_gain": head_gain, "expert_input": expert_input, "input_gain": input_gain, "specialist_choices": specialist_choices, "route_weight": route_weight, "gate_weight": gate_weight, "up_weight": up_weight, "down_weight": down_weight}


NORM_EPS = 1e-06
ROPE_BASE = 10000.0
SWIGLU_ALPHA = 1.702
SWIGLU_LIMIT = 7.0

def rotate(values_in, positions):
    half_dim = values_in.shape[-1] // 2
    inverse = 1.0 / ROPE_BASE ** jnp.linspace(0.0, 1.0, half_dim, dtype=jnp.float32)
    angles = positions.astype(jnp.float32)[:, None] * inverse[None, :]
    rotation_cosine = jnp.cos(angles)[:, None, :]
    sine_part = jnp.sin(angles)[:, None, :]
    lower_half = values_in[..., :half_dim]
    upper_half = values_in[..., half_dim:]
    return jnp.concatenate([lower_half * rotation_cosine - upper_half * sine_part, upper_half * rotation_cosine + lower_half * sine_part], axis=-1)

def head_norm(unscaled, gain):
    mean_removed = unscaled - lax.optimization_barrier(jnp.mean(unscaled, axis=-1, keepdims=True))
    scaled = mean_removed * lax.rsqrt(lax.optimization_barrier(jnp.mean(mean_removed * mean_removed, axis=-1, keepdims=True)) + NORM_EPS)
    return (scaled * gain).astype(jnp.bfloat16)

def clamped_unit(gate_value, up_value):
    bounded = jnp.minimum(gate_value, SWIGLU_LIMIT)
    linear = jnp.clip(up_value, -SWIGLU_LIMIT, SWIGLU_LIMIT)
    return bounded * jax.nn.sigmoid(SWIGLU_ALPHA * bounded) * (linear + 1.0)

def retention_block(state, inputs):
    query_block, key_block, value_block, decay_block, block_index = inputs
    positions = block_index * BLK + jnp.arange(BLK, dtype=jnp.int32)
    rot_query = rotate(query_block.astype(jnp.float32), positions).astype(jnp.bfloat16)
    rot_key = (rotate(key_block.astype(jnp.float32), positions) * DH ** (-0.5)).astype(jnp.bfloat16)
    within = jnp.cumsum(decay_block, axis=0)
    scores = jnp.einsum('qhd,khd->hqk', rot_query.astype(jnp.float32), rot_key.astype(jnp.float32))
    spread_amount = within.T[:, :, None] - within.T[:, None, :]
    causal = jnp.arange(BLK)[:, None] >= jnp.arange(BLK)[None, :]
    weights = jnp.where(causal[None], scores * jnp.exp(jnp.minimum(spread_amount, 0.0)), 0.0).astype(jnp.bfloat16)
    inside = jnp.einsum('hqk,khe->qhe', weights.astype(jnp.float32), value_block.astype(jnp.float32))
    leading = rot_query.astype(jnp.float32) * jnp.exp(within)[:, :, None]
    carried_part = jnp.einsum('qhd,hde->qhe', leading, state, precision=lax.Precision.HIGHEST)
    closing = within[-1]
    trailing = rot_key.astype(jnp.float32) * jnp.exp(closing[None, :] - within)[:, :, None]
    state = jnp.exp(closing)[:, None, None] * state + jnp.einsum('khd,khe->hde', trailing, value_block.astype(jnp.float32), precision=lax.Precision.HIGHEST)
    return (state, inside + carried_part)

def reference(query_heads, key_heads, value_heads, log_decay, head_gain, expert_input, input_gain, specialist_choices, route_weight, gate_weight, up_weight, down_weight):
    block_count = SEQUENCE_LENGTH // BLK
    block_shape = (block_count, BLK, HEADS, DH)
    gain_heads = head_gain.reshape(HEADS, DH)

    def mixer_step(state, inputs):
        state, unscaled = retention_block(state, inputs)
        return (state, head_norm(unscaled, gain_heads).reshape(BLK, HEADS * DH))
    zero_state = jnp.zeros((HEADS, DH, DH), jnp.float32)
    _, mixed = lax.scan(mixer_step, zero_state, (query_heads.reshape(block_shape), key_heads.reshape(block_shape), value_heads.reshape(block_shape), log_decay.reshape(block_count, BLK, HEADS), jnp.arange(block_count, dtype=jnp.int32)))
    mixer_out = mixed.reshape(SEQUENCE_LENGTH, HEADS * DH)
    inputs_f = expert_input.astype(jnp.float32)
    normed_in = (inputs_f * lax.rsqrt(lax.optimization_barrier(jnp.mean(inputs_f * inputs_f, axis=-1, keepdims=True)) + NORM_EPS) * input_gain).astype(jnp.bfloat16)
    flattened_routes = specialist_choices.reshape(-1).astype(jnp.int32)
    flat_weight = route_weight.reshape(-1)
    route_token = (jnp.arange(flattened_routes.shape[0], dtype=jnp.int32) // TOP_K).astype(jnp.int32)
    row_limit = N_EP * N_TP * CAP
    slice_count = N_TP // EXP_DEV
    slice_width = FF // slice_count

    def per_expert(totals, expert_id):
        matched = jnp.nonzero(flattened_routes == expert_id, size=row_limit, fill_value=0)[0].astype(jnp.int32)
        alive_mask = (jnp.arange(row_limit) < jnp.sum((flattened_routes == expert_id).astype(jnp.int32))).astype(jnp.float32)
        tokens_hit = route_token[matched]
        picked_rows = normed_in[tokens_hit]
        first_unit = (expert_id * FF).astype(jnp.int32)
        gate_cols = lax.dynamic_slice_in_dim(gate_weight, first_unit, FF, 1)
        up_cols = lax.dynamic_slice_in_dim(up_weight, first_unit, FF, 1)
        down_rows = lax.dynamic_slice_in_dim(down_weight, first_unit, FF, 0)
        gate_value = jnp.dot(picked_rows, gate_cols, preferred_element_type=jnp.float32)
        up_value = jnp.dot(picked_rows, up_cols, preferred_element_type=jnp.float32)
        hidden = clamped_unit(gate_value, up_value).astype(jnp.bfloat16)
        hidden_split = hidden.reshape(row_limit, slice_count, slice_width).astype(jnp.float32)
        down_split = down_rows.reshape(slice_count, slice_width, D).astype(jnp.float32)
        slice_parts = jnp.einsum('ntf,tfd->ntd', hidden_split, down_split).astype(jnp.bfloat16)
        slice_parts = lax.optimization_barrier(slice_parts)
        expert_value = lax.optimization_barrier(jnp.sum(slice_parts.astype(jnp.float32), axis=1)).astype(jnp.bfloat16)
        expert_value = lax.optimization_barrier(expert_value)
        scaled = expert_value.astype(jnp.float32) * (flat_weight[matched] * alive_mask)[:, None]
        return (totals.at[tokens_hit].add(scaled), None)
    totals, _ = lax.scan(per_expert, jnp.zeros((TOKENS_B, D), jnp.float32), jnp.arange(EXPERTS, dtype=jnp.int32))
    expert_out = totals.astype(jnp.bfloat16)
    return (mixer_out, expert_out)
```

```python
import functools

import jax
import jax.numpy as jnp
from jax import lax
from jax.experimental import pallas as pl
from jax.experimental.pallas import tpu as pltpu
from jax.sharding import PartitionSpec as P

EXP_DEV = 2
BLK = 512


NORM_EPS = 1e-06
ROPE_BASE = 10000.0
SWIGLU_ALPHA = 1.702
SWIGLU_LIMIT = 7.0


def table(positions, half_dim):
    inverse = 1.0 / ROPE_BASE ** jnp.linspace(0.0, 1.0, half_dim, dtype=jnp.float32)
    angles = positions.astype(jnp.float32)[:, None] * inverse[None, :]
    return jnp.cos(angles), jnp.sin(angles)


def block_tables(cos_ref, sin_ref, block_cos_ref, block_sin_ref):
    cos, sin = cos_ref[...], sin_ref[...]
    block_cos, block_sin = block_cos_ref[0], block_sin_ref[0]
    return cos * block_cos - sin * block_sin, sin * block_cos + cos * block_sin


def turned(ref, first, half, cos, sin, scale):
    low = ref[:, first : first + half].astype(jnp.float32)
    high = ref[:, first + half : first + 2 * half].astype(jnp.float32)
    a = low * cos - high * sin
    b = high * cos + low * sin
    if scale is not None:
        a, b = a * scale, b * scale
    return a.astype(jnp.bfloat16), b.astype(jnp.bfloat16)


def down_lanes(row, lanes):
    return jnp.broadcast_to(row, (lanes, row.shape[1])).T


def states_kernel(heads, k_ref, v_ref, w_ref, cos_ref, sin_ref, bc_ref, bs_ref, enter_ref, last_ref, held):
    block = pl.program_id(0)

    @pl.when(block == 0)
    def _():
        held[...] = jnp.zeros_like(held)

    dim = k_ref.shape[1] // heads
    half = dim // 2
    cos, sin = block_tables(cos_ref, sin_ref, bc_ref, bs_ref)
    for h in range(heads):
        enter_ref[0, h] = held[h]
        row = w_ref[0, h : h + 1, :]
        closing = row[:, row.shape[1] - 1 :]
        fade = down_lanes(jnp.exp(closing - row), half)
        a, b = turned(k_ref, h * dim, half, cos, sin, dim ** (-0.5))
        trailing = jnp.concatenate(
            [
                (a.astype(jnp.float32) * fade).astype(jnp.bfloat16),
                (b.astype(jnp.float32) * fade).astype(jnp.bfloat16),
            ],
            axis=1,
        )
        added = lax.dot_general(
            trailing,
            v_ref[:, h * dim : (h + 1) * dim],
            (((0,), (0,)), ((), ())),
            preferred_element_type=jnp.float32,
        )
        held[h] = jnp.exp(closing) * held[h] + added
    last_ref[...] = held[...]


def retain_kernel(
    heads, q_ref, k_ref, v_ref, w_ref, start_ref, cos_ref, sin_ref, bc_ref, bs_ref, enter_ref, carried_ref, gain_ref, out_ref
):
    dim = q_ref.shape[1] // heads
    half = dim // 2
    rows = q_ref.shape[0]
    part = rows // 2
    cos, sin = block_tables(cos_ref, sin_ref, bc_ref, bs_ref)
    ids_n = lax.broadcasted_iota(jnp.int32, (part, part), 0)
    ids_m = lax.broadcasted_iota(jnp.int32, (part, part), 1)
    causal = ids_n >= ids_m
    for h in range(heads):
        first = h * dim
        row = w_ref[0, h : h + 1, :]
        column = down_lanes(row, half)
        lead = jnp.exp(column)
        qa, qb = turned(q_ref, first, half, cos, sin, None)
        ka, kb = turned(k_ref, first, half, cos, sin, dim ** (-0.5))
        query = jnp.concatenate([qa, qb], axis=1)
        key = jnp.concatenate([ka, kb], axis=1)
        leading = jnp.concatenate(
            [
                (qa.astype(jnp.float32) * lead).astype(jnp.bfloat16),
                (qb.astype(jnp.float32) * lead).astype(jnp.bfloat16),
            ],
            axis=1,
        )
        before = jnp.exp(start_ref[0, h : h + 1, 0:1])
        state = (enter_ref[0, h] + before * carried_ref[h]).astype(jnp.bfloat16)
        value = v_ref[:, first : first + dim]
        for i in range(2):
            n = slice(i * part, (i + 1) * part)
            total = jnp.dot(leading[n], state, preferred_element_type=jnp.float32)
            for j in range(i + 1):
                m = slice(j * part, (j + 1) * part)
                scores = lax.dot_general(
                    query[n], key[m], (((1,), (1,)), ((), ())), preferred_element_type=jnp.float32
                )
                spread = jnp.concatenate([column[n]] * (part // half), axis=1) - row[:, m]
                weights = scores * jnp.exp(jnp.minimum(spread, 0.0))
                if i == j:
                    weights = jnp.where(causal, weights, 0.0)
                total = total + jnp.dot(
                    weights.astype(jnp.bfloat16), value[m], preferred_element_type=jnp.float32
                )
            removed = total - jnp.mean(total, axis=-1, keepdims=True)
            scaled = removed * lax.rsqrt(
                jnp.mean(removed * removed, axis=-1, keepdims=True) + NORM_EPS
            )
            out_ref[n, first : first + dim] = (scaled * gain_ref[:, first : first + dim]).astype(
                jnp.bfloat16
            )


def clamped_unit(gate_value, up_value):
    bounded = jnp.minimum(gate_value, SWIGLU_LIMIT)
    linear = jnp.clip(up_value, -SWIGLU_LIMIT, SWIGLU_LIMIT)
    return bounded * jax.nn.sigmoid(SWIGLU_ALPHA * bounded) * (linear + 1.0)


def expert_slice(rows, gate_part, up_part, down_part):
    gate_value = jnp.dot(rows, gate_part, preferred_element_type=jnp.float32)
    up_value = jnp.dot(rows, up_part, preferred_element_type=jnp.float32)
    hidden = clamped_unit(gate_value, up_value).astype(jnp.bfloat16)
    return jnp.dot(hidden, down_part, preferred_element_type=jnp.float32).astype(jnp.bfloat16)


def carried_in(local_state, device_decay):
    peers, index = lax.axis_size("ep"), lax.axis_index("ep")
    states = lax.all_gather(local_state, "ep")
    decays = lax.all_gather(device_decay, "ep")
    carried = jnp.zeros_like(local_state)
    for k in range(peers - 1):
        carried = jnp.where(
            k < index, jnp.exp(decays[k])[:, None, None] * carried + states[k], carried
        )
    return carried


def per_device(
    query_heads,
    key_heads,
    value_heads,
    log_decay,
    head_gain,
    expert_input,
    input_gain,
    specialist_choices,
    route_weight,
    gate_weight,
    up_weight,
    down_weight,
):
    seg_len, width = query_heads.shape
    heads = log_decay.shape[1]
    dim = width // heads
    half = dim // 2
    blocks = seg_len // BLK
    f32 = jnp.float32
    offset = lax.axis_index("ep") * seg_len

    within = jnp.cumsum(log_decay.T.reshape(heads, blocks, BLK), axis=2).transpose(1, 0, 2)
    closings = within[:, :, -1]
    starts = jnp.cumsum(closings, axis=0) - closings
    starts_wide = jnp.broadcast_to(starts[:, :, None], (blocks, heads, 128))
    cos, sin = table(jnp.arange(BLK, dtype=jnp.int32), half)
    block_cos, block_sin = table(offset + BLK * jnp.arange(blocks, dtype=jnp.int32), half)
    block_cos, block_sin = block_cos[:, None, :], block_sin[:, None, :]

    stream = pl.BlockSpec((BLK, width), lambda b: (b, 0))
    decay_spec = pl.BlockSpec((1, heads, BLK), lambda b: (b, 0, 0))
    fixed_spec = pl.BlockSpec((BLK, half), lambda b: (0, 0))
    turn_spec = pl.BlockSpec((1, 1, half), lambda b: (b, 0, 0))
    enter_spec = pl.BlockSpec((1, heads, dim, dim), lambda b: (b, 0, 0, 0))
    state_spec = pl.BlockSpec((heads, dim, dim), lambda b: (0, 0, 0))
    entering, local_state = pl.pallas_call(
        functools.partial(states_kernel, heads),
        grid=(blocks,),
        in_specs=[stream, stream, decay_spec, fixed_spec, fixed_spec, turn_spec, turn_spec],
        out_specs=[enter_spec, state_spec],
        out_shape=[
            jax.ShapeDtypeStruct((blocks, heads, dim, dim), f32),
            jax.ShapeDtypeStruct((heads, dim, dim), f32),
        ],
        scratch_shapes=[pltpu.VMEM((heads, dim, dim), f32)],
        compiler_params=pltpu.CompilerParams(vmem_limit_bytes=24 << 20),
        cost_estimate=pl.CostEstimate(
            flops=2 * seg_len * width * dim, bytes_accessed=12 * seg_len * width, transcendentals=0
        ),
        name="states",
    )(key_heads, value_heads, within, cos, sin, block_cos, block_sin)
    carried = carried_in(local_state, jnp.sum(closings, axis=0))
    mixer_out = pl.pallas_call(
        functools.partial(retain_kernel, heads),
        grid=(blocks,),
        in_specs=[
            stream,
            stream,
            stream,
            decay_spec,
            pl.BlockSpec((1, heads, 128), lambda b: (b, 0, 0)),
            fixed_spec,
            fixed_spec,
            turn_spec,
            turn_spec,
            enter_spec,
            state_spec,
            pl.BlockSpec((1, width), lambda b: (0, 0)),
        ],
        out_specs=stream,
        out_shape=jax.ShapeDtypeStruct((seg_len, width), jnp.bfloat16),
        compiler_params=pltpu.CompilerParams(vmem_limit_bytes=32 << 20),
        cost_estimate=pl.CostEstimate(
            flops=6 * seg_len * width * dim, bytes_accessed=24 * seg_len * width, transcendentals=0
        ),
        name="retain",
    )(
        query_heads,
        key_heads,
        value_heads,
        within,
        starts_wide,
        cos,
        sin,
        block_cos,
        block_sin,
        entering,
        carried,
        head_gain[None, :],
    )

    tok_count, model_dim = expert_input.shape
    top_count = specialist_choices.shape[1]
    ep_size = lax.axis_size("ep")
    tp_size = lax.axis_size("tp")
    group_size = tp_size // EXP_DEV
    expert_count = EXP_DEV * ep_size
    capacity = tok_count * top_count // expert_count + 1
    while ep_size * capacity % 8:
        capacity += 1
    slots = expert_count * capacity
    inputs_f = expert_input.astype(f32)
    normed_in = (
        inputs_f
        * lax.rsqrt(jnp.mean(inputs_f * inputs_f, axis=-1, keepdims=True) + NORM_EPS)
        * input_gain
    ).astype(jnp.bfloat16)
    experts = jnp.arange(expert_count, dtype=jnp.int32)
    picks = specialist_choices[:, :, None] == experts[None, None, :]
    named = jnp.sum(picks.astype(jnp.bfloat16), axis=1)
    earlier = (
        jnp.arange(tok_count, dtype=jnp.int32)[:, None]
        > jnp.arange(tok_count, dtype=jnp.int32)[None, :]
    ).astype(jnp.bfloat16)
    rank = jnp.dot(earlier, named, preferred_element_type=f32).astype(jnp.int32)
    slot_of = experts[None, :] * capacity + rank
    slot_index = jnp.sum(jnp.where(picks, slot_of[:, None, :], 0), axis=2)
    places = slot_index[:, :, None] == jnp.arange(slots, dtype=jnp.int32)[None, None, :]
    dispatch_matrix = jnp.any(places, axis=1).astype(jnp.bfloat16)
    outgoing = lax.dot_general(
        dispatch_matrix, normed_in, (((0,), (0,)), ((), ())), preferred_element_type=f32
    ).astype(jnp.bfloat16)
    outgoing = outgoing.reshape(ep_size, EXP_DEV, capacity, model_dim)
    arrived = lax.all_to_all(outgoing, "ep", split_axis=0, concat_axis=2, tiled=True)[0]
    row_count = arrived.shape[1]
    tp_index = lax.axis_index("tp")
    my_group = tp_index // group_size
    partners = [(t, (t + group_size) % tp_size) for t in range(tp_size)]
    groups = [
        list(range(g * group_size, (g + 1) * group_size)) for g in range(EXP_DEV)
    ]
    own = lax.dynamic_index_in_dim(arrived, my_group, 0, keepdims=False)
    away = lax.dynamic_index_in_dim(arrived, 1 - my_group, 0, keepdims=False)
    met = lax.ppermute(away, "tp", partners)
    pair = jnp.concatenate([own, met], axis=0)
    mine = lax.all_gather(pair, "tp", axis=0, tiled=True, axis_index_groups=groups)
    partials = expert_slice(mine, gate_weight, up_weight, down_weight)
    values = lax.psum_scatter(
        partials, "tp", scatter_dimension=0, axis_index_groups=groups, tiled=True
    )
    home = values[:row_count]
    back = lax.ppermute(values[row_count:], "tp", partners)
    first = jnp.where(my_group == 0, home, back)
    second = jnp.where(my_group == 0, back, home)
    value_blocks = jnp.stack([first, second]).reshape(EXP_DEV, ep_size, capacity, model_dim)
    returned = lax.all_to_all(value_blocks, "ep", split_axis=1, concat_axis=0, tiled=True)
    flat_results = returned.reshape(slots, model_dim)
    mix = jnp.sum(jnp.where(places, route_weight[:, :, None], 0.0), axis=1)
    expert_out = jnp.dot(
        mix, flat_results.astype(f32), precision=lax.Precision.HIGHEST
    ).astype(jnp.bfloat16)
    return (mixer_out, expert_out)


def solution(mesh):
    in_specs = (
        P("ep", "tp"),
        P("ep", "tp"),
        P("ep", "tp"),
        P("ep", "tp"),
        P("tp"),
        P(("ep", "tp"), None),
        P(),
        P(("ep", "tp"), None),
        P(("ep", "tp"), None),
        P(None, ("ep", "tp")),
        P(None, ("ep", "tp")),
        P(("ep", "tp"), None),
    )
    out_specs = (P("ep", "tp"), P(("ep", "tp"), None))
    return jax.shard_map(
        per_device, mesh=mesh, in_specs=in_specs, out_specs=out_specs, check_vma=False
    )
```

```python
import functools

import jax
import jax.numpy as jnp
from jax import lax
from jax.experimental import pallas as pl
from jax.experimental.pallas import tpu as pltpu
from jax.sharding import PartitionSpec as P

EXP_DEV = 2
BLK = 512


NORM_EPS = 1e-06
ROPE_BASE = 10000.0
SWIGLU_ALPHA = 1.702
SWIGLU_LIMIT = 7.0


def table(positions, half_dim):
    inverse = 1.0 / ROPE_BASE ** jnp.linspace(0.0, 1.0, half_dim, dtype=jnp.float32)
    angles = positions.astype(jnp.float32)[:, None] * inverse[None, :]
    return jnp.cos(angles), jnp.sin(angles)


def block_tables(cos_ref, sin_ref, block_cos_ref, block_sin_ref):
    cos, sin = cos_ref[...], sin_ref[...]
    block_cos, block_sin = block_cos_ref[0], block_sin_ref[0]
    return cos * block_cos - sin * block_sin, sin * block_cos + cos * block_sin


def turned(ref, first, half, cos, sin, scale):
    low = ref[:, first : first + half].astype(jnp.float32)
    high = ref[:, first + half : first + 2 * half].astype(jnp.float32)
    a = low * cos - high * sin
    b = high * cos + low * sin
    if scale is not None:
        a, b = a * scale, b * scale
    return a.astype(jnp.bfloat16), b.astype(jnp.bfloat16)


def down_lanes(row, lanes):
    return jnp.broadcast_to(row, (lanes, row.shape[1])).T


def states_kernel(heads, k_ref, v_ref, w_ref, start_ref, cos_ref, sin_ref, bc_ref, bs_ref, enter_ref, last_ref, held):
    block = pl.program_id(0)

    @pl.when(block == 0)
    def _():
        held[...] = jnp.zeros_like(held)

    dim = k_ref.shape[1] // heads
    half = dim // 2
    cos, sin = block_tables(cos_ref, sin_ref, bc_ref, bs_ref)
    for h in range(heads):
        enter_ref[0, h] = held[h]
        row = w_ref[0, h : h + 1, :]
        closing = row[:, row.shape[1] - 1 :]
        fade = down_lanes(jnp.exp(closing - row), half)
        a, b = turned(k_ref, h * dim, half, cos, sin, dim ** (-0.5))
        trailing = jnp.concatenate(
            [
                (a.astype(jnp.float32) * fade).astype(jnp.bfloat16),
                (b.astype(jnp.float32) * fade).astype(jnp.bfloat16),
            ],
            axis=1,
        )
        added = lax.dot_general(
            trailing,
            v_ref[:, h * dim : (h + 1) * dim],
            (((0,), (0,)), ((), ())),
            preferred_element_type=jnp.float32,
        )
        held[h] = jnp.exp(closing) * held[h] + added
        passed = start_ref[0, h : h + 1, 0:1] + closing
        rough = passed.astype(jnp.bfloat16)
        rest = (passed - rough.astype(jnp.float32)).astype(jnp.bfloat16)
        extra = (last_ref.shape[1] - dim) // 2
        last_ref[h, dim : dim + extra, :] = jnp.broadcast_to(rough, (extra, dim))
        last_ref[h, dim + extra :, :] = jnp.broadcast_to(rest, (extra, dim))
    last_ref[:, :dim, :] = held[...].astype(jnp.bfloat16)


def retain_kernel(
    heads, q_ref, k_ref, v_ref, w_ref, start_ref, cos_ref, sin_ref, bc_ref, bs_ref, enter_ref, carried_ref, gain_ref, out_ref
):
    dim = q_ref.shape[1] // heads
    half = dim // 2
    rows = q_ref.shape[0]
    part = rows // 2
    cos, sin = block_tables(cos_ref, sin_ref, bc_ref, bs_ref)
    ids_n = lax.broadcasted_iota(jnp.int32, (part, part), 0)
    ids_m = lax.broadcasted_iota(jnp.int32, (part, part), 1)
    causal = ids_n >= ids_m
    for h in range(heads):
        first = h * dim
        row = w_ref[0, h : h + 1, :]
        column = down_lanes(row, half)
        lead = jnp.exp(column)
        qa, qb = turned(q_ref, first, half, cos, sin, None)
        ka, kb = turned(k_ref, first, half, cos, sin, dim ** (-0.5))
        query = jnp.concatenate([qa, qb], axis=1)
        key = jnp.concatenate([ka, kb], axis=1)
        leading = jnp.concatenate(
            [
                (qa.astype(jnp.float32) * lead).astype(jnp.bfloat16),
                (qb.astype(jnp.float32) * lead).astype(jnp.bfloat16),
            ],
            axis=1,
        )
        before = jnp.exp(start_ref[0, h : h + 1, 0:1])
        state = (enter_ref[0, h] + before * carried_ref[h]).astype(jnp.bfloat16)
        value = v_ref[:, first : first + dim]
        for i in range(2):
            n = slice(i * part, (i + 1) * part)
            total = jnp.dot(leading[n], state, preferred_element_type=jnp.float32)
            for j in range(i + 1):
                m = slice(j * part, (j + 1) * part)
                scores = lax.dot_general(
                    query[n], key[m], (((1,), (1,)), ((), ())), preferred_element_type=jnp.float32
                )
                spread = jnp.concatenate([column[n]] * (part // half), axis=1) - row[:, m]
                weights = scores * jnp.exp(jnp.minimum(spread, 0.0))
                if i == j:
                    weights = jnp.where(causal, weights, 0.0)
                total = total + jnp.dot(
                    weights.astype(jnp.bfloat16), value[m], preferred_element_type=jnp.float32
                )
            removed = total - jnp.mean(total, axis=-1, keepdims=True)
            scaled = removed * lax.rsqrt(
                jnp.mean(removed * removed, axis=-1, keepdims=True) + NORM_EPS
            )
            out_ref[n, first : first + dim] = (scaled * gain_ref[:, first : first + dim]).astype(
                jnp.bfloat16
            )


def clamped_unit(gate_value, up_value):
    bounded = jnp.minimum(gate_value, SWIGLU_LIMIT)
    linear = jnp.clip(up_value, -SWIGLU_LIMIT, SWIGLU_LIMIT)
    return bounded * jax.nn.sigmoid(SWIGLU_ALPHA * bounded) * (linear + 1.0)


def expert_slice(rows, gate_part, up_part, down_part):
    gate_value = jnp.dot(rows, gate_part, preferred_element_type=jnp.float32)
    up_value = jnp.dot(rows, up_part, preferred_element_type=jnp.float32)
    hidden = clamped_unit(gate_value, up_value).astype(jnp.bfloat16)
    return jnp.dot(hidden, down_part, preferred_element_type=jnp.float32).astype(jnp.bfloat16)


def carried_in(local, dim):
    peers = lax.axis_size("ep")
    carried = jnp.zeros((local.shape[0], dim, dim), jnp.float32)
    for step in range(peers - 1, 0, -1):
        got = lax.ppermute(local, "ep", [(e, e + step) for e in range(peers - step)])
        got = got.astype(jnp.float32)
        passed = got[:, dim : dim + 1] + got[:, dim + 16 : dim + 17]
        carried = got[:, :dim] + jnp.exp(passed) * carried
    return carried


def swap(x, distance):
    size = lax.axis_size("tp")
    return lax.ppermute(x, "tp", [(t, t ^ distance) for t in range(size)])


def per_device(
    query_heads,
    key_heads,
    value_heads,
    log_decay,
    head_gain,
    expert_input,
    input_gain,
    specialist_choices,
    route_weight,
    gate_weight,
    up_weight,
    down_weight,
):
    seg_len, width = query_heads.shape
    heads = log_decay.shape[1]
    dim = width // heads
    half = dim // 2
    blocks = seg_len // BLK
    f32 = jnp.float32
    offset = lax.axis_index("ep") * seg_len

    within = jnp.cumsum(log_decay.T.reshape(heads, blocks, BLK), axis=2).transpose(1, 0, 2)
    closings = within[:, :, -1]
    starts = jnp.cumsum(closings, axis=0) - closings
    starts_wide = jnp.broadcast_to(starts[:, :, None], (blocks, heads, 128))
    cos, sin = table(jnp.arange(BLK, dtype=jnp.int32), half)
    block_cos, block_sin = table(offset + BLK * jnp.arange(blocks, dtype=jnp.int32), half)
    block_cos, block_sin = block_cos[:, None, :], block_sin[:, None, :]

    stream = pl.BlockSpec((BLK, width), lambda b: (b, 0))
    decay_spec = pl.BlockSpec((1, heads, BLK), lambda b: (b, 0, 0))
    start_spec = pl.BlockSpec((1, heads, 128), lambda b: (b, 0, 0))
    last_spec = pl.BlockSpec((heads, dim + 32, dim), lambda b: (0, 0, 0))
    fixed_spec = pl.BlockSpec((BLK, half), lambda b: (0, 0))
    turn_spec = pl.BlockSpec((1, 1, half), lambda b: (b, 0, 0))
    enter_spec = pl.BlockSpec((1, heads, dim, dim), lambda b: (b, 0, 0, 0))
    state_spec = pl.BlockSpec((heads, dim, dim), lambda b: (0, 0, 0))
    entering, local_state = pl.pallas_call(
        functools.partial(states_kernel, heads),
        grid=(blocks,),
        in_specs=[stream, stream, decay_spec, start_spec, fixed_spec, fixed_spec, turn_spec, turn_spec],
        out_specs=[enter_spec, last_spec],
        out_shape=[
            jax.ShapeDtypeStruct((blocks, heads, dim, dim), f32),
            jax.ShapeDtypeStruct((heads, dim + 32, dim), jnp.bfloat16),
        ],
        scratch_shapes=[pltpu.VMEM((heads, dim, dim), f32)],
        compiler_params=pltpu.CompilerParams(vmem_limit_bytes=60 << 20),
        cost_estimate=pl.CostEstimate(
            flops=2 * seg_len * width * dim, bytes_accessed=12 * seg_len * width, transcendentals=0
        ),
        name="states",
    )(key_heads, value_heads, within, starts_wide, cos, sin, block_cos, block_sin)
    tok_count, model_dim = expert_input.shape
    top_count = specialist_choices.shape[1]
    ep_size = lax.axis_size("ep")
    tp_size = lax.axis_size("tp")
    group_size = tp_size // EXP_DEV
    expert_count = EXP_DEV * ep_size
    capacity = tok_count * top_count // expert_count + 1
    while ep_size * capacity % 8:
        capacity += 1
    slots = expert_count * capacity
    inputs_f = expert_input.astype(f32)
    normed_in = (
        inputs_f
        * lax.rsqrt(jnp.mean(inputs_f * inputs_f, axis=-1, keepdims=True) + NORM_EPS)
        * input_gain
    ).astype(jnp.bfloat16)
    experts = jnp.arange(expert_count, dtype=jnp.int32)
    picks = specialist_choices[:, :, None] == experts[None, None, :]
    named = jnp.sum(picks.astype(jnp.bfloat16), axis=1)
    earlier = (
        jnp.arange(tok_count, dtype=jnp.int32)[:, None]
        > jnp.arange(tok_count, dtype=jnp.int32)[None, :]
    ).astype(jnp.bfloat16)
    rank = jnp.dot(earlier, named, preferred_element_type=f32).astype(jnp.int32)
    tp_index = lax.axis_index("tp")
    my_group = tp_index // group_size
    turned_by = (experts % EXP_DEV + EXP_DEV - my_group) % EXP_DEV
    slot_of = (experts - experts % EXP_DEV + turned_by)[None, :] * capacity + rank
    slot_index = jnp.sum(jnp.where(picks, slot_of[:, None, :], 0), axis=2)
    places = slot_index[:, :, None] == jnp.arange(slots, dtype=jnp.int32)[None, None, :]
    dispatch_matrix = jnp.any(places, axis=1).astype(jnp.bfloat16)
    outgoing = lax.dot_general(
        dispatch_matrix, normed_in, (((0,), (0,)), ((), ())), preferred_element_type=f32
    ).astype(jnp.bfloat16)
    outgoing = outgoing.reshape(ep_size, EXP_DEV, capacity, model_dim)
    arrived = lax.all_to_all(outgoing, "ep", split_axis=0, concat_axis=2, tiled=True)[0]
    arrived, local_state = lax.optimization_barrier((arrived, local_state))
    carried = carried_in(local_state, dim)
    row_count = arrived.shape[1]
    own, away = arrived[0], arrived[1]
    partners = [(t, (t + group_size) % tp_size) for t in range(tp_size)]
    if group_size == 4:
        met = lax.ppermute(away, "tp", partners)
        met, carried = lax.optimization_barrier((met, carried))
        own_far = swap(own, 2)
        met_far = swap(met, 2)
        held = jnp.concatenate([own, own_far, met, met_far], axis=0)
        mine = jnp.concatenate([held, swap(held, 1)], axis=0)
        partials = expert_slice(mine, gate_weight, up_weight, down_weight)
        near = 4 * row_count
        summed = partials[:near].astype(f32) + swap(partials[near:], 1).astype(f32)
        own_sum, own_other, met_sum, met_other = (
            summed[k * row_count : (k + 1) * row_count] for k in range(4)
        )
        met_got = swap(met_other.astype(jnp.bfloat16), 2)
        met_total = (met_sum + met_got.astype(f32)).astype(jnp.bfloat16)
        own_got = swap(own_other.astype(jnp.bfloat16), 2)
        back = lax.ppermute(met_total, "tp", partners)
        own_got, back = lax.optimization_barrier((own_got, back))
        home = (own_sum + own_got.astype(f32)).astype(jnp.bfloat16)
    else:
        groups = [list(range(g * group_size, (g + 1) * group_size)) for g in range(EXP_DEV)]
        met = lax.ppermute(away, "tp", partners)
        met, carried = lax.optimization_barrier((met, carried))
        pair = jnp.concatenate([own, met], axis=0)
        mine = lax.all_gather(pair, "tp", axis=0, tiled=True, axis_index_groups=groups)
        partials = expert_slice(mine, gate_weight, up_weight, down_weight)
        values = lax.psum_scatter(
            partials, "tp", scatter_dimension=0, axis_index_groups=groups, tiled=True
        )
        home = values[:row_count]
        back = lax.ppermute(values[row_count:], "tp", partners)
    mixer_out = pl.pallas_call(
        functools.partial(retain_kernel, heads),
        grid=(blocks,),
        in_specs=[
            stream,
            stream,
            stream,
            decay_spec,
            start_spec,
            fixed_spec,
            fixed_spec,
            turn_spec,
            turn_spec,
            enter_spec,
            state_spec,
            pl.BlockSpec((1, width), lambda b: (0, 0)),
        ],
        out_specs=stream,
        out_shape=jax.ShapeDtypeStruct((seg_len, width), jnp.bfloat16),
        compiler_params=pltpu.CompilerParams(vmem_limit_bytes=60 << 20),
        cost_estimate=pl.CostEstimate(
            flops=6 * seg_len * width * dim, bytes_accessed=24 * seg_len * width, transcendentals=0
        ),
        name="retain",
    )(
        query_heads,
        key_heads,
        value_heads,
        within,
        starts_wide,
        cos,
        sin,
        block_cos,
        block_sin,
        entering,
        carried,
        head_gain[None, :],
    )
    value_blocks = jnp.stack([home, back]).reshape(EXP_DEV, ep_size, capacity, model_dim)
    value_blocks, mixer_out = lax.optimization_barrier((value_blocks, mixer_out))
    returned = lax.all_to_all(value_blocks, "ep", split_axis=1, concat_axis=0, tiled=True)
    flat_results = returned.reshape(slots, model_dim)
    mix = jnp.sum(jnp.where(places, route_weight[:, :, None], 0.0), axis=1)
    expert_out = jnp.dot(
        mix, flat_results.astype(f32), precision=lax.Precision.HIGHEST
    ).astype(jnp.bfloat16)
    return (mixer_out, expert_out)


def solution(mesh):
    in_specs = (
        P("ep", "tp"),
        P("ep", "tp"),
        P("ep", "tp"),
        P("ep", "tp"),
        P("tp"),
        P(("ep", "tp"), None),
        P(),
        P(("ep", "tp"), None),
        P(("ep", "tp"), None),
        P(None, ("ep", "tp")),
        P(None, ("ep", "tp")),
        P(("ep", "tp"), None),
    )
    out_specs = (P("ep", "tp"), P(("ep", "tp"), None))
    return jax.shard_map(
        per_device, mesh=mesh, in_specs=in_specs, out_specs=out_specs, check_vma=False
    )
```
